32 devices in a mesh: ep: 16 (over z, y, core), tp: 2 (over x).
Axes of the slice: x: 2, y: 2, z: 4, core: 2. Of those that a mesh axis runs over, the one named last changes fastest.
Arguments:
- tokens: bfloat16 [256, 2048], P('ep'), may hold values from -6 to 6
- recur_state: float32 [256, 8, 128, 128], P('ep', 'tp'), may hold values from -0.4 to 0.4
- attn_gain: float32 [2048], replicated, may hold values from 0.1 to 1.9
- query_weight: bfloat16 [2048, 1024], P(None, 'tp'), may hold values from -0.125 to 0.125
- key_weight: bfloat16 [2048, 1024], P(None, 'tp'), may hold values from -0.125 to 0.125
- value_weight: bfloat16 [2048, 1024], P(None, 'tp'), may hold values from -0.125 to 0.125
- outgate_weight: bfloat16 [2048, 1024], P(None, 'tp'), may hold values from -0.125 to 0.125
- beta_weight: bfloat16 [2048, 8], replicated, may hold values from -0.125 to 0.125
- decay_weight: bfloat16 [2048, 8], replicated, may hold values from -0.125 to 0.125
- decay_rate: float32 [8], replicated, may hold values from 0.05 to 2
- head_gain: float32 [128], replicated, may hold values from 0.1 to 1.9
- output_weight: bfloat16 [1024, 2048], P('tp'), may hold values from -0.1875 to 0.1875
- ffn_gain: float32 [2048], replicated, may hold values from 0.1 to 1.9
- routes: int32 [256, 2], P('ep'), may hold values from 0 to 3, all different within a row; in each aligned block of 16 rows (0 to 15, 16 to 31, ...) at most 16 rows name the same one
- route_weight: float32 [256, 2], P('ep'), may hold values from 0.2 to 1
- expert_gate: bfloat16 [16, 2048, 1024], P('ep', None, 'tp'), may hold values from -0.125 to 0.125
- expert_up: bfloat16 [16, 2048, 1024], P('ep', None, 'tp'), may hold values from -0.125 to 0.125
- expert_down: bfloat16 [16, 1024, 2048], P('ep', 'tp'), may hold values from -0.09375 to 0.09375
Outputs:
- mixed: bfloat16 [256, 2048], P('ep', 'tp')
- new_state: float32 [256, 8, 128, 128], P('ep', 'tp')
The draws below stay inside these ranges and needn't reach their ends.
Inputs may be any that keep to these rules, and one draw needn't show every extreme that they name: `routes`: each row names 2 different experts; in each aligned block of 16 rows no expert is named by more than 16 rows.
All inputs are finite; a program needn't handle non-finite values.
Results may differ from the reference program's by a relative error of at most 0.014.
Values may be sent and summed in bfloat16 or wider, within the bound.
A program may use at most 64 MiB of HBM per device.

```python
import math
import jax
import jax.numpy as jnp
import numpy as np
from jax import lax

D = 2048
H = 8
HEAD = 128
FF_E = 4096
TOP = 2
SEQ_DEV = 16
TOKENS = 256
EXPERTS = 4
FF_PART = 1024
CAP = 16
N_EP = 16


def levels(key, shape, cuts, low, largest):
    def one(dim, shards_of):
        steps = jax.random.uniform(jax.random.fold_in(jax.random.fold_in(key, 6), dim), (shards_of,), jnp.float32, low / len(cuts), largest / len(cuts))
        return jnp.repeat(jnp.exp(steps), shape[dim] // shards_of).reshape((-1,) + (1,) * (len(shape) - dim - 1))

    level = one(*cuts[0])
    for cut in cuts[1:]:
        level = level * one(*cut)
    return level


def shared_out(rng, own, number, rows, count, top, reach, lean):
    order = jax.random.permutation(rng, count)
    crowded, ordinary = load_shares(count, rows * top, reach, lean, True), load_shares(count, rows * top, reach, lean, False)
    places = jnp.arange(count)

    def named(sizes, offset_by):
        used = int((sizes > 0).sum())
        fixed = max(1, used // 4)
        passed = fixed + (places - fixed + offset_by * (used - fixed)) % max(1, count - fixed)
        return jnp.zeros((count,), jnp.int32).at[order[jnp.where(places < fixed, places, passed)]].set(jnp.asarray(sizes, jnp.int32))

    sizes = jnp.where(number % 4 == 0, named(crowded, number // 4), named(ordinary, number - number // 4 - 1))
    mixed = jax.random.permutation(jax.random.fold_in(own, 3), count)
    donor, sink = mixed[0:count // 2 * 2:2], mixed[1:count // 2 * 2:2]
    room = jnp.minimum(sizes[donor] - 1, reach - sizes[sink]) // 2
    room = jnp.where((donor == order[0]) | (sink == order[0]) | (sizes[sink] == 0), 0, jnp.maximum(room, 0))
    passed = jax.random.randint(jax.random.fold_in(own, 4), (count // 2,), 0, 1 << 20) % (room + 1)
    sizes = sizes.at[donor].add(-passed).at[sink].add(passed)
    members = jnp.searchsorted(jnp.cumsum(sizes), jnp.arange(rows * top), side="right").astype(jnp.int32)
    listing = members.reshape(top, rows).T
    listing = listing[jax.random.permutation(jax.random.fold_in(own, 1), rows)]
    offset_by = jax.random.randint(jax.random.fold_in(own, 2), (rows, 1), 0, top)
    return jnp.take_along_axis(listing, (jnp.arange(top)[None, :] + offset_by) % top, axis=1)


def load_shares(amount, total, most, lean, full):
    loads = [(1 << 20) // math.isqrt(grade ** lean) + 1 for grade in range(1, amount + 1)]
    largest = most if full else min(most, max(-(-total // amount), total * loads[0] // sum(loads)))
    least = 1 if total - largest >= amount - 1 else 0
    counts, spare = [largest] + [least] * (amount - 1), total - largest - least * (amount - 1)
    while spare > 0:
        candidates = [i for i in range(1, amount) if counts[i] < largest] or [i for i in range(1, amount) if counts[i] < most]
        pool, budget = sum([loads[i] for i in candidates]), spare
        for i in candidates:
            extra = min(most - counts[i], max(1, budget * loads[i] // pool), spare)
            counts[i] = counts[i] + extra
            spare = spare - extra
    return np.array(counts)


def scatter_about(own_key, shape, width, limit, shards=(), kind=jnp.bfloat16):
    values = width * jax.random.normal(own_key, shape, jnp.float32)
    if shards:
        values = values * levels(own_key, shape, shards, -0.22, 0.18)
    return jnp.clip(values, -limit, limit).astype(kind)


def setup_inputs(seed: int = 0) -> dict:
    splits = jax.random.split(jax.random.key(seed), 19)
    tokens = scatter_about(splits[0], (TOKENS, D), 1.0, 6.0, ((0, 16),))
    recur_state = scatter_about(splits[1], (TOKENS, H, HEAD, HEAD), 0.05, 0.4, ((0, 16), (1, 2)), jnp.float32)
    attn_gain = jnp.clip(1.0 + 0.18 * jax.random.normal(splits[2], (D,), jnp.float32), 0.1, 1.9)
    query_weight = scatter_about(splits[3], (D, H * HEAD), D ** -0.5, 0.125, ((1, 2),))
    key_weight = scatter_about(splits[4], (D, H * HEAD), D ** -0.5, 0.125, ((1, 2),))
    value_weight = scatter_about(splits[5], (D, H * HEAD), D ** -0.5, 0.125, ((1, 2),))
    outgate_weight = scatter_about(splits[6], (D, H * HEAD), D ** -0.5, 0.125, ((1, 2),))
    beta_weight = scatter_about(splits[7], (D, H), D ** -0.5, 0.125)
    decay_weight = scatter_about(splits[8], (D, H), D ** -0.5, 0.125)
    decay_rate = jnp.clip(jnp.exp(jax.random.uniform(splits[9], (H,), jnp.float32, math.log(0.05), math.log(2.0))), 0.05, 2.0)
    head_gain = jnp.clip(1.0 + 0.18 * jax.random.normal(splits[10], (HEAD,), jnp.float32), 0.1, 1.9)
    output_weight = scatter_about(splits[11], (H * HEAD, D), (H * HEAD) ** -0.5, 0.1875, ((0, 2),))
    ffn_gain = jnp.clip(1.0 + 0.18 * jax.random.normal(splits[12], (D,), jnp.float32), 0.1, 1.9)
    routes_keys = jax.random.split(jax.random.fold_in(splits[13], 1), TOKENS // SEQ_DEV)
    routes_turns = jax.random.permutation(jax.random.fold_in(splits[13], 3), TOKENS // SEQ_DEV)
    routes = jax.vmap(lambda own, number: shared_out(jax.random.fold_in(splits[13], 2), own, number, SEQ_DEV, EXPERTS, TOP, CAP, 2))(routes_keys, routes_turns).reshape((TOKENS, TOP))
    route_weight = jnp.clip(jnp.exp(math.log(1.0) - 1.609438 * jax.random.uniform(splits[14], (TOKENS, TOP), jnp.float32) ** levels(splits[14], (TOKENS, TOP), ((0, 16),), -0.2, 0.2)), 0.2, 1.0)
    expert_gate = scatter_about(splits[15], (4 * EXPERTS, D, FF_PART), D ** -0.5, 0.125, ((0, 16), (2, 2)))
    expert_up = scatter_about(splits[16], (4 * EXPERTS, D, FF_PART), D ** -0.5, 0.125, ((0, 16), (2, 2)))
    expert_down = scatter_about(splits[17], (4 * EXPERTS, FF_PART, D), FF_E ** -0.5, 0.09375, ((0, 16), (1, 2)))
    return {"tokens": tokens, "recur_state": recur_state, "attn_gain": attn_gain, "query_weight": query_weight, "key_weight": key_weight, "value_weight": value_weight, "outgate_weight": outgate_weight, "beta_weight": beta_weight, "decay_weight": decay_weight, "decay_rate": decay_rate, "head_gain": head_gain, "output_weight": output_weight, "ffn_gain": ffn_gain, "routes": routes, "route_weight": route_weight, "expert_gate": expert_gate, "expert_up": expert_up, "expert_down": expert_down}


EPS = 1e-06

def rms_scale(values, gain):
    return values * lax.rsqrt(lax.optimization_barrier(jnp.mean(values * values, axis=-1, keepdims=True)) + EPS) * gain

def unit_rows(values):
    return values * lax.rsqrt(lax.optimization_barrier(jnp.sum(values * values, axis=-1, keepdims=True)) + EPS)

def slot_targets(group_routes, experts, capacity):
    flat = group_routes.reshape(-1)
    onehot = (flat[:, None] == jnp.arange(experts, dtype=jnp.int32)[None, :]).astype(jnp.int32)
    running = jnp.cumsum(onehot, axis=0)
    position = lax.optimization_barrier(jnp.sum(running * onehot, axis=1)) - 1
    return (flat * capacity + position).reshape(group_routes.shape).astype(jnp.int32)

def reference(tokens, recur_state, attn_gain, query_weight, key_weight, value_weight, outgate_weight, beta_weight, decay_weight, decay_rate, head_gain, output_weight, ffn_gain, routes, route_weight, expert_gate, expert_up, expert_down):
    f32 = jnp.float32
    bf16 = jnp.bfloat16
    highest = lax.Precision.HIGHEST
    normed = rms_scale(tokens.astype(f32), attn_gain).astype(bf16)
    qproj = jnp.dot(normed, query_weight, preferred_element_type=f32).astype(bf16)
    kproj = jnp.dot(normed, key_weight, preferred_element_type=f32).astype(bf16)
    vproj = jnp.dot(normed, value_weight, preferred_element_type=f32).astype(bf16)
    zproj = jnp.dot(normed, outgate_weight, preferred_element_type=f32).astype(bf16)
    strength = jax.nn.sigmoid(jnp.dot(normed, beta_weight, preferred_element_type=f32))
    fading = jnp.exp(-decay_rate * jax.nn.softplus(jnp.dot(normed, decay_weight, preferred_element_type=f32)))

    def split_heads(proj):
        return proj.astype(f32).reshape(TOKENS, H, HEAD)
    query = unit_rows(jax.nn.silu(split_heads(qproj))) * HEAD ** (-0.5)
    keyvec = unit_rows(jax.nn.silu(split_heads(kproj)))
    value = jax.nn.silu(split_heads(vproj))
    recall = jnp.einsum('thd,thde->the', keyvec, recur_state, precision=highest)
    written = (strength[..., None] * keyvec)[..., :, None] * (value - fading[..., None] * recall)[..., None, :]
    new_state = fading[..., None, None] * recur_state + written
    readout = jnp.einsum('thd,thde->the', query, new_state, precision=highest)
    headed = (rms_scale(readout, head_gain) * jax.nn.silu(split_heads(zproj))).reshape(TOKENS, H * HEAD).astype(bf16)
    branch = jnp.dot(headed, output_weight, preferred_element_type=f32).astype(bf16)
    resid = (tokens.astype(f32) + branch.astype(f32)).astype(bf16)
    ffn_in = rms_scale(resid.astype(f32), ffn_gain).astype(bf16)
    grouped = ffn_in.reshape(N_EP, SEQ_DEV, D)
    group_routes = routes.reshape(N_EP, SEQ_DEV, TOP)
    group_weight = route_weight.reshape(N_EP, SEQ_DEV, TOP)
    targets = jax.vmap(lambda block: slot_targets(block, EXPERTS, CAP))(group_routes)
    slot_ids = jnp.arange(EXPERTS * CAP, dtype=jnp.int32)
    select = jnp.any(targets[:, None, :, :] == slot_ids[None, :, None, None], axis=-1).astype(f32)
    buffers = jnp.einsum('gst,gtd->gsd', select, grouped.astype(f32), precision=highest).astype(bf16)
    per_expert = buffers.reshape(N_EP, EXPERTS, CAP, D).transpose(1, 0, 2, 3).reshape(EXPERTS, N_EP * CAP, D)
    gates = expert_gate.reshape(EXPERTS, 4, D, FF_PART)
    ups = expert_up.reshape(EXPERTS, 4, D, FF_PART)
    downs = expert_down.reshape(EXPERTS, 4, FF_PART, D)

    def run_expert(operands):
        rows, gate_set, up_set, down_set = operands
        total = jnp.zeros((rows.shape[0], D), f32)
        for slice_idx in range(4):
            gated = jnp.dot(rows, gate_set[slice_idx], preferred_element_type=f32)
            lifted = jnp.dot(rows, up_set[slice_idx], preferred_element_type=f32)
            hidden = (jax.nn.silu(gated) * lifted).astype(bf16)
            piece = lax.optimization_barrier(jnp.dot(hidden, down_set[slice_idx], preferred_element_type=f32).astype(bf16))
            total = total + piece.astype(f32)
        return total
    results = lax.map(run_expert, (per_expert, gates, ups, downs))
    results = results.reshape(EXPERTS, N_EP, CAP, D).transpose(1, 0, 2, 3).reshape(N_EP, EXPERTS * CAP, D)
    combine = jnp.zeros((N_EP, SEQ_DEV, EXPERTS * CAP), f32)
    for choice_idx in range(TOP):
        match = (targets[..., choice_idx, None] == slot_ids).astype(f32)
        combine = combine + group_weight[..., choice_idx, None] * match
    moe = jnp.einsum('gts,gsd->gtd', combine, results, precision=highest).reshape(TOKENS, D)
    mixed = (resid.astype(f32) + moe).astype(bf16)
    return (mixed, new_state)
```

```python
import functools

import jax
import jax.numpy as jnp
from jax import lax
from jax.experimental import pallas as pl
from jax.experimental.pallas import tpu as pltpu
from jax.sharding import PartitionSpec as P

EPS = 1e-06
MESH = pl.DeviceIdType.MESH
F32 = jnp.float32
BF16 = jnp.bfloat16
SIDE = 128


def silu(values):
    return values / (1.0 + jnp.exp(-values))


def unit_rows(values):
    return values * lax.rsqrt(jnp.sum(values * values, axis=-1, keepdims=True) + EPS)


def rms_scale(values, gain):
    return values * lax.rsqrt(jnp.mean(values * values, axis=-1, keepdims=True) + EPS) * gain


def mixer_kernel(
    tok_ref, gain_ref, bt_ref, dt_ref, rate_ref, hg_ref,
    wk_hbm, wq_hbm, wv_hbm, st_hbm, wz_hbm, wo_hbm,
    out_ref, ns_hbm,
    wk, wq, wv, wz, wo, st, ns, w_sem, s_sem, n_sem,
):
    heads, seqs, hd = st.shape[0], st.shape[1], st.shape[2]

    def fetch(src, dst, i):
        copy = pltpu.make_async_copy(src, dst, w_sem.at[i])
        copy.start()
        return copy

    ck, cq, cv = fetch(wk_hbm, wk, 0), fetch(wq_hbm, wq, 1), fetch(wv_hbm, wv, 2)
    cs = []
    for j in range(heads):
        copy = pltpu.make_async_copy(st_hbm.at[:, j], st.at[j], s_sem.at[j])
        copy.start()
        cs.append(copy)
    cz, co = fetch(wz_hbm, wz, 3), fetch(wo_hbm, wo, 4)

    normed = rms_scale(tok_ref[...].astype(F32), gain_ref[...]).astype(BF16)
    dims = (((1,), (1,)), ((), ()))
    bl = lax.dot_general(normed, bt_ref[...], dims, preferred_element_type=F32)
    dl = lax.dot_general(normed, dt_ref[...], dims, preferred_element_type=F32)
    strength = 1.0 / (1.0 + jnp.exp(-bl))
    softplus = jnp.maximum(dl, 0.0) + jnp.log1p(jnp.exp(-jnp.abs(dl)))
    fading = jnp.exp(-rate_ref[...] * softplus)
    first = lax.axis_index("tp") * heads
    head_ids = lax.broadcasted_iota(jnp.int32, bl.shape, 1)

    def own(values, j):
        return jnp.sum(jnp.where(head_ids == first + j, values, 0.0), axis=1, keepdims=True)

    def project(copy, ref):
        copy.wait()
        return jnp.dot(normed, ref[...], preferred_element_type=F32).astype(BF16).astype(F32)

    kp, qp, vp = project(ck, wk), project(cq, wq), project(cv, wv)
    row2 = lax.broadcasted_iota(jnp.int32, (2 * seqs, hd), 0)
    row1 = lax.broadcasted_iota(jnp.int32, (seqs, hd), 0)
    outs, readouts = [], []
    for j in range(heads):
        cut = slice(j * hd, (j + 1) * hd)
        kh = unit_rows(silu(kp[:, cut]))
        qh = unit_rows(silu(qp[:, cut])) * hd ** (-0.5)
        vh = silu(vp[:, cut])
        both = jnp.concatenate([kh, qh], axis=0)
        spread = jnp.concatenate(
            [jnp.where((row2 == t) | (row2 == t + seqs), both, 0.0).astype(BF16) for t in range(seqs)],
            axis=1,
        )
        cs[j].wait()
        held = st[j].reshape(seqs * hd, hd).astype(BF16)
        read = jnp.dot(spread, held, preferred_element_type=F32)
        fd, bt = own(fading, j), own(strength, j)
        delta = bt * (vh - fd * read[:seqs])
        readouts.append(fd * read[seqs:] + jnp.sum(kh * qh, axis=-1, keepdims=True) * delta)
        kt = kh.T.astype(BF16)
        fdb = jnp.broadcast_to(fd, (seqs, hd))
        step = 4
        for t0 in range(0, seqs, step):
            block = jnp.concatenate(
                [jnp.where(row1 == t, delta, 0.0).astype(BF16) for t in range(t0, t0 + step)], axis=1
            )
            written = jnp.dot(kt, block, preferred_element_type=F32)
            for i in range(step):
                t = t0 + i
                ns[j, t] = fdb[t : t + 1] * st[j, t] + written[:, i * hd : (i + 1) * hd]
        copy = pltpu.make_async_copy(ns.at[j], ns_hbm.at[:, j], n_sem.at[j])
        copy.start()
        outs.append(copy)
    zp = project(cz, wz)
    headed = jnp.concatenate(
        [
            (rms_scale(readouts[j], hg_ref[...]) * silu(zp[:, j * hd : (j + 1) * hd])).astype(BF16)
            for j in range(heads)
        ],
        axis=1,
    )
    co.wait()
    out_ref[...] = jnp.dot(headed, wo[...], preferred_element_type=F32).astype(BF16)
    for copy in outs:
        copy.wait()


def expert_kernel(
    nz, ny, lanes,
    tok_ref, part_ref, gain_ref, routes_ref, rw_ref, wg_hbm, wu_hbm, wd_hbm,
    out_ref,
    wg, wu, wd, tpb, rows, resid, cs, cr, pf, xs, xr, qf, ys, yr, zs, zr,
    w_sem, tp_s, tp_r, ag_s, ag_r, c_s, c_r, x_s, x_r, y_s, y_r, z_s, z_r,
):
    seqs, width = tok_ref.shape
    dl = width // lanes
    zy = nz * ny
    ep, tp = lax.axis_index("ep"), lax.axis_index("tp")
    c = lax.rem(ep, 2)
    y = lax.rem(ep // 2, ny)
    z = ep // (2 * ny)
    other = 1 - c

    fetched = []
    for i, (src, dst) in enumerate(((wg_hbm, wg), (wu_hbm, wu), (wd_hbm, wd))):
        copy = pltpu.make_async_copy(src.at[0], dst, w_sem.at[i])
        copy.start()
        fetched.append(copy)

    def device(zz, yy, cc):
        return {"ep": (zz * ny + yy) * 2 + cc}

    def turn(base, step, size):
        return lax.rem(base + step, size)

    partner = device(z, y, other)
    barrier = pltpu.get_barrier_semaphore()
    peers = [partner]
    peers += [{"tp": turn(tp, d, lanes)} for d in range(1, lanes)]
    peers += [device(z, turn(y, d, ny), c) for d in range(1, ny)]
    peers += [device(turn(z, d, nz), y, c) for d in range(1, nz)]
    for peer in peers:
        pl.semaphore_signal(barrier, inc=1, device_id=peer, device_id_type=MESH)
    pl.semaphore_wait(barrier, len(peers))

    started = []

    def remote(src, dst, s_sem, r_sem, dev):
        return pltpu.make_async_remote_copy(
            src_ref=src, dst_ref=dst, send_sem=s_sem, recv_sem=r_sem, device_id=dev, device_id_type=MESH
        )

    def send(src, dst, s_sem, r_sem, dev):
        copy = remote(src, dst, s_sem, r_sem, dev)
        copy.start()
        started.append(copy)

    def arrive(dst, s_sem, r_sem):
        remote(dst, dst, s_sem, r_sem, partner).wait_recv()

    for d in range(1, lanes):
        send(part_ref, tpb.at[tp], tp_s.at[d], tp_r.at[tp], {"tp": turn(tp, d, lanes)})

    routes, weights = routes_ref[...], rw_ref[...]
    side = lax.broadcasted_iota(jnp.int32, (seqs, SIDE), 1)
    expert_of = jnp.where(side >= SIDE // 2, side - SIDE // 2, side)
    combine = jnp.zeros((seqs, SIDE), F32)
    for k in range(routes.shape[1]):
        combine = combine + jnp.where(expert_of == routes[:, k : k + 1], weights[:, k : k + 1], 0.0)
    high = combine.astype(BF16).astype(F32)
    packed = jnp.where(side >= SIDE // 2, combine - high, high).astype(BF16)

    branch = part_ref[...].astype(F32)
    for d in range(1, lanes):
        src = turn(tp, d, lanes)
        arrive(tpb.at[src], tp_s.at[0], tp_r.at[src])
        branch = branch + tpb[src].astype(F32)
    res = (tok_ref[...].astype(F32) + branch.astype(BF16).astype(F32)).astype(BF16).astype(F32)
    for j in range(lanes):
        resid[j] = res[:, j * dl : (j + 1) * dl]

    def place(zz, yy, cc):
        return cc * zy + zz * ny + yy

    mine = place(z, y, c)
    rows[mine, :, :width] = rms_scale(res, gain_ref[...]).astype(BF16)
    rows[mine, :, width:] = packed

    count = [0]

    def pass_on(p, dev):
        send(rows.at[p], rows.at[p], ag_s.at[count[0]], ag_r.at[p], dev)
        count[0] += 1

    def landed(p):
        arrive(rows.at[p], ag_s.at[0], ag_r.at[p])

    near = sorted(range(1, nz), key=lambda d: (min(d, nz - d), d))
    for d in reversed(near):
        pass_on(mine, device(turn(z, d, nz), y, c))
    for d in range(1, ny):
        pass_on(mine, device(z, turn(y, d, ny), c))
    pass_on(mine, partner)
    for dz in near:
        p = place(turn(z, dz, nz), y, c)
        landed(p)
        for d in range(1, ny):
            pass_on(p, device(z, turn(y, d, ny), c))
        pass_on(p, partner)
    for dz in [0] + near:
        for d in range(1, ny):
            p = place(turn(z, dz, nz), turn(y, d, ny), c)
            landed(p)
            pass_on(p, partner)

    my_expert = ep // 4
    lane_id = lax.broadcasted_iota(jnp.int32, (zy * seqs, SIDE), 1)

    def hidden_of(half):
        block = rows[pl.ds(half * zy, zy)].reshape(zy * seqs, width + SIDE)
        x = block[:, :width]
        pick = (lane_id == my_expert) | (lane_id == my_expert + SIDE // 2)
        share = jnp.sum(jnp.where(pick, block[:, width:].astype(F32), 0.0), axis=1, keepdims=True)
        gated = jnp.dot(x, wg[...], preferred_element_type=F32)
        lifted = jnp.dot(x, wu[...], preferred_element_type=F32)
        return (silu(gated) * lifted * share).astype(BF16)

    fetched[0].wait()
    fetched[1].wait()
    hidden_own = hidden_of(c)
    for dz in [0] + near:
        for d in range(ny):
            landed(place(turn(z, dz, nz), turn(y, d, ny), other))
    hidden_far = hidden_of(other)
    fetched[2].wait()
    for j in range(lanes):
        cut = slice(j * dl, (j + 1) * dl)
        far = jnp.dot(hidden_far, wd[:, cut], preferred_element_type=F32)
        cs[j] = far.astype(BF16).reshape(zy, seqs, dl)

    order = list(reversed(near)) + [0]

    def chunk(k):
        zt = turn(z, k, nz)
        return zt, pl.ds(zt * ny, ny)

    for k in order:
        _, at = chunk(k)
        send(cs.at[:, at], cr.at[:, at], c_s.at[k], c_r.at[k], partner)
    for j in range(lanes):
        cut = slice(j * dl, (j + 1) * dl)
        near_half = jnp.dot(hidden_own, wd[:, cut], preferred_element_type=F32)
        pf[j] = near_half.reshape(zy, seqs, dl)
    for k in order:
        _, at = chunk(k)
        arrive(cr.at[:, at], c_s.at[k], c_r.at[k])
        for d in range(1, lanes):
            jt = turn(tp, d, lanes)
            xs[jt, at] = (pf[jt, at] + cr[jt, at].astype(F32)).astype(BF16)
            send(xs.at[jt, at], xr.at[tp, at], x_s.at[d, k], x_r.at[tp, k], {"tp": jt})
        pf[tp, at] = pf[tp, at] + cr[tp, at].astype(F32)
    for k in order:
        zt, at = chunk(k)
        total = pf[tp, at]
        for d in range(1, lanes):
            src = turn(tp, d, lanes)
            arrive(xr.at[src, at], x_s.at[d, k], x_r.at[src, k])
            total = total + xr[src, at].astype(F32)
        qf[at] = total
        for d in range(1, ny):
            yt = turn(y, d, ny)
            ys[zt * ny + yt] = qf[zt * ny + yt].astype(BF16)
            send(ys.at[zt * ny + yt], yr.at[zt * ny + y], y_s.at[d, k], y_r.at[y, k], device(z, yt, c))
    for k in order:
        zt, at = chunk(k)
        total = qf[zt * ny + y]
        for d in range(1, ny):
            src = turn(y, d, ny)
            arrive(yr.at[zt * ny + src], y_s.at[d, k], y_r.at[src, k])
            total = total + yr[zt * ny + src].astype(F32)
        if k:
            zs[zt] = total.astype(BF16)
            send(zs.at[zt], zr.at[z], z_s.at[k], z_r.at[z], device(zt, y, c))
    for d in near:
        src = turn(z, d, nz)
        arrive(zr.at[src], z_s.at[d], z_r.at[src])
        total = total + zr[src].astype(F32)
    out_ref[...] = (resid[tp] + total).astype(BF16)
    for copy in started:
        copy.wait_send()


def local(
    tokens, recur_state, attn_gain, query_weight, key_weight, value_weight, outgate_weight,
    beta_weight, decay_weight, decay_rate, head_gain, output_weight, ffn_gain, routes,
    route_weight, expert_gate, expert_up, expert_down,
):
    seqs, width = tokens.shape
    heads, hd = recur_state.shape[1], recur_state.shape[2]
    groups, lanes = lax.axis_size("ep"), lax.axis_size("tp")
    ny = 1
    while ny * ny * 4 <= groups // 2:
        ny *= 2
    nz = groups // (2 * ny)
    zy = nz * ny
    dl = width // lanes
    hidden = expert_gate.shape[2]
    vmem = pl.BlockSpec(memory_space=pltpu.VMEM)
    any_ = pl.BlockSpec(memory_space=pl.ANY)
    dma = pltpu.SemaphoreType.DMA
    inner = heads * hd
    part, new_state = pl.pallas_call(
        mixer_kernel,
        name="mixer",
        out_shape=(
            jax.ShapeDtypeStruct((seqs, width), BF16),
            jax.ShapeDtypeStruct(recur_state.shape, F32),
        ),
        in_specs=[vmem] * 6 + [any_] * 6,
        out_specs=(vmem, any_),
        scratch_shapes=[pltpu.VMEM((width, inner), BF16)] * 4
        + [
            pltpu.VMEM((inner, width), BF16),
            pltpu.VMEM((heads, seqs, hd, hd), F32),
            pltpu.VMEM((heads, seqs, hd, hd), F32),
            dma((5,)),
            dma((heads,)),
            dma((heads,)),
        ],
        compiler_params=pltpu.CompilerParams(vmem_limit_bytes=60 * 1024 * 1024),
    )(
        tokens, attn_gain[None], beta_weight.T, decay_weight.T, decay_rate[None], head_gain[None],
        key_weight, query_weight, value_weight, recur_state, outgate_weight, output_weight,
    )
    mixed = pl.pallas_call(
        functools.partial(expert_kernel, nz, ny, lanes),
        name="experts",
        out_shape=jax.ShapeDtypeStruct((seqs, dl), BF16),
        in_specs=[vmem] * 5 + [any_] * 3,
        out_specs=vmem,
        scratch_shapes=[
            pltpu.VMEM((width, hidden), BF16),
            pltpu.VMEM((width, hidden), BF16),
            pltpu.VMEM((hidden, width), BF16),
            pltpu.VMEM((lanes, seqs, width), BF16),
            pltpu.VMEM((groups, seqs, width + SIDE), BF16),
            pltpu.VMEM((lanes, seqs, dl), F32),
            pltpu.VMEM((lanes, zy, seqs, dl), BF16),
            pltpu.VMEM((lanes, zy, seqs, dl), BF16),
            pltpu.VMEM((lanes, zy, seqs, dl), F32),
            pltpu.VMEM((lanes, zy, seqs, dl), BF16),
            pltpu.VMEM((lanes, zy, seqs, dl), BF16),
            pltpu.VMEM((zy, seqs, dl), F32),
            pltpu.VMEM((zy, seqs, dl), BF16),
            pltpu.VMEM((zy, seqs, dl), BF16),
            pltpu.VMEM((nz, seqs, dl), BF16),
            pltpu.VMEM((nz, seqs, dl), BF16),
            dma((3,)),
            dma((lanes,)),
            dma((lanes,)),
            dma((groups,)),
            dma((groups,)),
            dma((nz,)),
            dma((nz,)),
            dma((lanes, nz)),
            dma((lanes, nz)),
            dma((ny, nz)),
            dma((ny, nz)),
            dma((nz,)),
            dma((nz,)),
        ],
        compiler_params=pltpu.CompilerParams(
            collective_id=0, has_side_effects=True, vmem_limit_bytes=60 * 1024 * 1024
        ),
    )(
        tokens, part, ffn_gain[None], routes, route_weight, expert_gate, expert_up, expert_down,
    )
    return mixed, new_state


def solution(mesh):
    return jax.shard_map(
        local,
        mesh=mesh,
        in_specs=(
            P("ep", None),
            P("ep", "tp", None, None),
            P(),
            P(None, "tp"),
            P(None, "tp"),
            P(None, "tp"),
            P(None, "tp"),
            P(),
            P(),
            P(),
            P(),
            P("tp", None),
            P(),
            P("ep", None),
            P("ep", None),
            P("ep", None, "tp"),
            P("ep", None, "tp"),
            P("ep", "tp", None),
        ),
        out_specs=(P("ep", "tp"), P("ep", "tp", None, None)),
        check_vma=False,
    )
```

```python
import functools

import jax
import jax.numpy as jnp
from jax import lax
from jax.experimental import pallas as pl
from jax.experimental.pallas import tpu as pltpu
from jax.sharding import PartitionSpec as P

EPS = 1e-06
MESH = pl.DeviceIdType.MESH
F32 = jnp.float32
BF16 = jnp.bfloat16
SIDE = 128


def silu(values):
    return values / (1.0 + jnp.exp(-values))


def unit_rows(values):
    return values * lax.rsqrt(jnp.sum(values * values, axis=-1, keepdims=True) + EPS)


def rms_scale(values, gain):
    return values * lax.rsqrt(jnp.mean(values * values, axis=-1, keepdims=True) + EPS) * gain


def mixer_kernel(
    tok_ref, gain_ref, bt_ref, dt_ref, rate_ref, hg_ref,
    wk_hbm, wq_hbm, wv_hbm, st_hbm, wz_hbm, wo_hbm,
    out_ref, ns_hbm,
    wk, wq, wv, wz, wo, st, ns, w_sem, s_sem, n_sem,
):
    heads, seqs, hd = st.shape[0], st.shape[1], st.shape[2]

    def fetch(src, dst, i):
        copy = pltpu.make_async_copy(src, dst, w_sem.at[i])
        copy.start()
        return copy

    ck, cq, cv = fetch(wk_hbm, wk, 0), fetch(wq_hbm, wq, 1), fetch(wv_hbm, wv, 2)
    cs = []
    for j in range(heads):
        copy = pltpu.make_async_copy(st_hbm.at[:, j], st.at[j], s_sem.at[j])
        copy.start()
        cs.append(copy)
    cz, co = fetch(wz_hbm, wz, 3), fetch(wo_hbm, wo, 4)

    normed = rms_scale(tok_ref[...].astype(F32), gain_ref[...]).astype(BF16)
    dims = (((1,), (1,)), ((), ()))
    bl = lax.dot_general(normed, bt_ref[...], dims, preferred_element_type=F32)
    dl = lax.dot_general(normed, dt_ref[...], dims, preferred_element_type=F32)
    strength = 1.0 / (1.0 + jnp.exp(-bl))
    softplus = jnp.maximum(dl, 0.0) + jnp.log1p(jnp.exp(-jnp.abs(dl)))
    fading = jnp.exp(-rate_ref[...] * softplus)
    first = lax.axis_index("tp") * heads
    head_ids = lax.broadcasted_iota(jnp.int32, bl.shape, 1)

    def own(values, j):
        return jnp.sum(jnp.where(head_ids == first + j, values, 0.0), axis=1, keepdims=True)

    def project(copy, ref):
        copy.wait()
        return jnp.dot(normed, ref[...], preferred_element_type=F32).astype(BF16).astype(F32)

    kp, qp, vp = project(ck, wk), project(cq, wq), project(cv, wv)
    row2 = lax.broadcasted_iota(jnp.int32, (2 * seqs, hd), 0)
    row1 = lax.broadcasted_iota(jnp.int32, (seqs, hd), 0)
    outs, readouts = [], []
    for j in range(heads):
        cut = slice(j * hd, (j + 1) * hd)
        kh = unit_rows(silu(kp[:, cut]))
        qh = unit_rows(silu(qp[:, cut])) * hd ** (-0.5)
        vh = silu(vp[:, cut])
        both = jnp.concatenate([kh, qh], axis=0)
        spread = jnp.concatenate(
            [jnp.where((row2 == t) | (row2 == t + seqs), both, 0.0).astype(BF16) for t in range(seqs)],
            axis=1,
        )
        cs[j].wait()
        held = st[j].reshape(seqs * hd, hd).astype(BF16)
        read = jnp.dot(spread, held, preferred_element_type=F32)
        fd, bt = own(fading, j), own(strength, j)
        delta = bt * (vh - fd * read[:seqs])
        readouts.append(fd * read[seqs:] + jnp.sum(kh * qh, axis=-1, keepdims=True) * delta)
        kt = kh.T.astype(BF16)
        fdb = jnp.broadcast_to(fd, (seqs, hd))
        step = 4
        for t0 in range(0, seqs, step):
            block = jnp.concatenate(
                [jnp.where(row1 == t, delta, 0.0).astype(BF16) for t in range(t0, t0 + step)], axis=1
            )
            written = jnp.dot(kt, block, preferred_element_type=F32)
            for i in range(step):
                t = t0 + i
                ns[j, t] = fdb[t : t + 1] * st[j, t] + written[:, i * hd : (i + 1) * hd]
        copy = pltpu.make_async_copy(ns.at[j], ns_hbm.at[:, j], n_sem.at[j])
        copy.start()
        outs.append(copy)
    zp = project(cz, wz)
    headed = jnp.concatenate(
        [
            (rms_scale(readouts[j], hg_ref[...]) * silu(zp[:, j * hd : (j + 1) * hd])).astype(BF16)
            for j in range(heads)
        ],
        axis=1,
    )
    co.wait()
    out_ref[...] = jnp.dot(headed, wo[...], preferred_element_type=F32).astype(BF16)
    for copy in outs:
        copy.wait()


def expert_kernel(
    nz, ny, lanes,
    tok_ref, part_ref, gain_ref, routes_ref, rw_ref, wg_hbm, wu_hbm, wd_hbm,
    out_ref,
    wg, wu, wd, tpb, rows, resid, cs, cr, pf, xs, xr, qf, ys, yr, ybs, ybr, zs, zr,
    w_sem, tp_s, tp_r, ag_s, ag_r, c_s, c_r, x_s, x_r, y_s, y_r, z_s, z_r,
):
    seqs, width = tok_ref.shape
    dl = width // lanes
    zy = nz * ny
    ep, tp = lax.axis_index("ep"), lax.axis_index("tp")
    c = lax.rem(ep, 2)
    y = lax.rem(ep // 2, ny)
    z = ep // (2 * ny)
    other = 1 - c

    fetched = []
    for i, (src, dst) in enumerate(((wg_hbm, wg), (wu_hbm, wu), (wd_hbm, wd))):
        copy = pltpu.make_async_copy(src.at[0], dst, w_sem.at[i])
        copy.start()
        fetched.append(copy)

    def device(zz, yy, cc):
        return {"ep": (zz * ny + yy) * 2 + cc}

    def turn(base, step, size):
        return lax.rem(base + step, size)

    partner = device(z, y, other)
    barrier = pltpu.get_barrier_semaphore()
    peers = [partner]
    peers += [{"tp": turn(tp, d, lanes)} for d in range(1, lanes)]
    peers += [device(z, turn(y, d, ny), c) for d in range(1, ny)]
    peers += [device(turn(z, d, nz), y, c) for d in range(1, nz)]
    for peer in peers:
        pl.semaphore_signal(barrier, inc=1, device_id=peer, device_id_type=MESH)
    pl.semaphore_wait(barrier, len(peers))

    started = []

    def remote(src, dst, s_sem, r_sem, dev):
        return pltpu.make_async_remote_copy(
            src_ref=src, dst_ref=dst, send_sem=s_sem, recv_sem=r_sem, device_id=dev, device_id_type=MESH
        )

    def send(src, dst, s_sem, r_sem, dev):
        copy = remote(src, dst, s_sem, r_sem, dev)
        copy.start()
        started.append(copy)

    def arrive(dst, s_sem, r_sem):
        remote(dst, dst, s_sem, r_sem, partner).wait_recv()

    for d in range(1, lanes):
        send(part_ref, tpb.at[tp], tp_s.at[d], tp_r.at[tp], {"tp": turn(tp, d, lanes)})

    routes, weights = routes_ref[...].astype(F32), rw_ref[...]
    top = routes.shape[0]
    pad = jnp.zeros((8 - 2 * top % 8, seqs), F32)
    turned = jnp.concatenate([routes, weights, pad], axis=0).T
    side = lax.broadcasted_iota(jnp.int32, (seqs, SIDE), 1)
    expert_of = jnp.where(side >= SIDE // 2, side - SIDE // 2, side).astype(F32)
    combine = jnp.zeros((seqs, SIDE), F32)
    for k in range(top):
        weight = turned[:, top + k : top + k + 1]
        combine = combine + jnp.where(expert_of == turned[:, k : k + 1], weight, 0.0)
    high = combine.astype(BF16).astype(F32)
    packed = jnp.where(side >= SIDE // 2, combine - high, high).astype(BF16)

    branch = part_ref[...].astype(F32)
    for d in range(1, lanes):
        src = turn(tp, d, lanes)
        arrive(tpb.at[src], tp_s.at[0], tp_r.at[src])
        branch = branch + tpb[src].astype(F32)
    res = (tok_ref[...].astype(F32) + branch.astype(BF16).astype(F32)).astype(BF16).astype(F32)
    for j in range(lanes):
        resid[j] = res[:, j * dl : (j + 1) * dl]

    def place(zz, yy, cc):
        return cc * zy + zz * ny + yy

    mine = place(z, y, c)
    rows[mine, :, :width] = rms_scale(res, gain_ref[...]).astype(BF16)
    rows[mine, :, width:] = packed

    count = [0]
    half = nz // 2
    low = z < half
    base = jnp.where(low, 0, half)
    edge = jnp.where(low, half - 1, half)
    far_edge = jnp.where(low, half, half - 1)
    outward = jnp.where(low, 1, -1)
    at_edge = z == edge
    middle = width // 2
    pieces = (slice(0, middle), slice(middle, width + SIDE))

    def block(p, piece):
        return rows.at[p, :, pieces[piece]]

    def pass_on(p, piece, dev):
        send(block(p, piece), block(p, piece), ag_s.at[count[0]], ag_r.at[piece, p], dev)
        count[0] += 1

    def landed(p, piece):
        arrive(block(p, piece), ag_s.at[0], ag_r.at[piece, p])

    def spread(p, piece):
        for d in range(1, ny):
            pass_on(p, piece, device(z, turn(y, d, ny), c))
        pass_on(p, piece, partner)

    mates = [base + lax.rem(z - base + d, half) for d in range(1, half)]
    both = range(len(pieces))
    for piece in both:
        pass_on(mine, piece, device(far_edge, y, c))
        for mate in mates:
            pass_on(mine, piece, device(mate, y, c))
        spread(mine, piece)
    for mate in mates:
        for piece in both:
            p = place(mate, y, c)
            landed(p, piece)
            spread(p, piece)
    relayed = []
    for i in range(half):
        for piece in both:
            p = place(far_edge + outward * i, y, c)
            landed(p, piece)
            for mate in mates:
                copy = remote(
                    block(p, piece), block(p, piece), ag_s.at[count[0]], ag_r.at[piece, p],
                    device(mate, y, c),
                )
                count[0] += 1
                relayed.append(copy)
                pl.when(at_edge)(copy.start)
            spread(p, piece)
    columns = [z] + mates + [far_edge + outward * i for i in range(half)]
    for zz in columns:
        for d in range(1, ny):
            for piece in both:
                p = place(zz, turn(y, d, ny), c)
                landed(p, piece)
                pass_on(p, piece, partner)

    my_expert = ep // 4
    lane_id = lax.broadcasted_iota(jnp.int32, (zy * seqs, SIDE), 1)

    def hidden_of(side_of):
        block = rows[pl.ds(side_of * zy, zy)].reshape(zy * seqs, width + SIDE)
        x = block[:, :width]
        pick = (lane_id == my_expert) | (lane_id == my_expert + SIDE // 2)
        share = jnp.sum(jnp.where(pick, block[:, width:].astype(F32), 0.0), axis=1, keepdims=True)
        gated = jnp.dot(x, wg[...], preferred_element_type=F32)
        lifted = jnp.dot(x, wu[...], preferred_element_type=F32)
        return (silu(gated) * lifted * share).astype(BF16)

    fetched[0].wait()
    fetched[1].wait()
    hidden_own = hidden_of(c)
    for d in range(ny):
        for zz in columns:
            for piece in both:
                landed(place(zz, turn(y, d, ny), other), piece)
    hidden_far = hidden_of(other)
    fetched[2].wait()
    targets = [lax.rem(z + outward * d + nz, nz) for d in range(nz - 1, -1, -1)]
    spans = [pl.ds(zt * ny, ny) for zt in targets]
    steps = range(nz)
    for j in range(lanes):
        cut = slice(j * dl, (j + 1) * dl)
        far = jnp.dot(hidden_far, wd[:, cut], preferred_element_type=F32)
        cs[j] = far.astype(BF16).reshape(zy, seqs, dl)
        for i in steps:
            send(cs.at[j, spans[i]], cr.at[j, spans[i]], c_s.at[j, i], c_r.at[j, i], partner)
    for j in range(lanes):
        cut = slice(j * dl, (j + 1) * dl)
        near_half = jnp.dot(hidden_own, wd[:, cut], preferred_element_type=F32)
        pf[j] = near_half.reshape(zy, seqs, dl)

    def first_tp(i):
        return i % 2 == 0

    tp_peers = [(d, turn(tp, d, lanes)) for d in range(1, lanes)]
    y_peers = [(d, turn(y, d, ny)) for d in range(1, ny)]
    for i in steps:
        zt, at = targets[i], spans[i]
        for j in range(lanes):
            arrive(cr.at[j, at], c_s.at[j, i], c_r.at[j, i])
        if first_tp(i):
            for d, jt in tp_peers:
                xs[jt, at] = (pf[jt, at] + cr[jt, at].astype(F32)).astype(BF16)
                send(xs.at[jt, at], xr.at[tp, at], x_s.at[d, i], x_r.at[tp, i], {"tp": jt})
            pf[tp, at] = pf[tp, at] + cr[tp, at].astype(F32)
        else:
            for d, yt in y_peers:
                row = zt * ny + yt
                ybs[:, row] = (pf[:, row] + cr[:, row].astype(F32)).astype(BF16)
                send(
                    ybs.at[:, row], ybr.at[:, zt * ny + y], y_s.at[d, i], y_r.at[y, i], device(z, yt, c)
                )
            row = zt * ny + y
            pf[:, row] = pf[:, row] + cr[:, row].astype(F32)
    for i in steps:
        zt, at = targets[i], spans[i]
        if first_tp(i):
            total = pf[tp, at]
            for d, src in tp_peers:
                arrive(xr.at[src, at], x_s.at[d, i], x_r.at[src, i])
                total = total + xr[src, at].astype(F32)
            qf[at] = total
            for d, yt in y_peers:
                row = zt * ny + yt
                ys[row] = qf[row].astype(BF16)
                send(ys.at[row], yr.at[zt * ny + y], y_s.at[d, i], y_r.at[y, i], device(z, yt, c))
        else:
            row = zt * ny + y
            total = pf[:, row]
            for d, src in y_peers:
                back = zt * ny + src
                arrive(ybr.at[:, back], y_s.at[d, i], y_r.at[src, i])
                total = total + ybr[:, back].astype(F32)
            pf[:, row] = total
            for d, jt in tp_peers:
                xs[jt, row] = pf[jt, row].astype(BF16)
                send(xs.at[jt, row], xr.at[tp, row], x_s.at[d, i], x_r.at[tp, i], {"tp": jt})
    for i in steps:
        zt = targets[i]
        row = zt * ny + y
        if first_tp(i):
            total = qf[row]
            for d, src in y_peers:
                back = zt * ny + src
                arrive(yr.at[back], y_s.at[d, i], y_r.at[src, i])
                total = total + yr[back].astype(F32)
        else:
            total = pf[tp, row]
            for d, src in tp_peers:
                arrive(xr.at[src, row], x_s.at[d, i], x_r.at[src, i])
                total = total + xr[src, row].astype(F32)
        if i < nz - 1:
            zs[zt] = total.astype(BF16)
            send(zs.at[zt], zr.at[z], z_s.at[i], z_r.at[z], device(zt, y, c))
    for d in range(1, nz):
        src = turn(z, d, nz)
        arrive(zr.at[src], z_s.at[0], z_r.at[src])
        total = total + zr[src].astype(F32)
    out_ref[...] = (resid[tp] + total).astype(BF16)
    for copy in started:
        copy.wait_send()
    for copy in relayed:
        pl.when(at_edge)(copy.wait_send)


def local(
    tokens, recur_state, attn_gain, query_weight, key_weight, value_weight, outgate_weight,
    beta_weight, decay_weight, decay_rate, head_gain, output_weight, ffn_gain, routes,
    route_weight, expert_gate, expert_up, expert_down,
):
    seqs, width = tokens.shape
    heads, hd = recur_state.shape[1], recur_state.shape[2]
    groups, lanes = lax.axis_size("ep"), lax.axis_size("tp")
    ny = 1
    while ny * ny * 4 <= groups // 2:
        ny *= 2
    nz = groups // (2 * ny)
    zy = nz * ny
    dl = width // lanes
    hidden = expert_gate.shape[2]
    vmem = pl.BlockSpec(memory_space=pltpu.VMEM)
    any_ = pl.BlockSpec(memory_space=pl.ANY)
    dma = pltpu.SemaphoreType.DMA
    inner = heads * hd
    part, new_state = pl.pallas_call(
        mixer_kernel,
        name="mixer",
        out_shape=(
            jax.ShapeDtypeStruct((seqs, width), BF16),
            jax.ShapeDtypeStruct(recur_state.shape, F32),
        ),
        in_specs=[vmem] * 6 + [any_] * 6,
        out_specs=(vmem, any_),
        scratch_shapes=[pltpu.VMEM((width, inner), BF16)] * 4
        + [
            pltpu.VMEM((inner, width), BF16),
            pltpu.VMEM((heads, seqs, hd, hd), F32),
            pltpu.VMEM((heads, seqs, hd, hd), F32),
            dma((5,)),
            dma((heads,)),
            dma((heads,)),
        ],
        compiler_params=pltpu.CompilerParams(vmem_limit_bytes=60 * 1024 * 1024),
    )(
        tokens, attn_gain[None], beta_weight.T, decay_weight.T, decay_rate[None], head_gain[None],
        key_weight, query_weight, value_weight, recur_state, outgate_weight, output_weight,
    )
    mixed = pl.pallas_call(
        functools.partial(expert_kernel, nz, ny, lanes),
        name="experts",
        out_shape=jax.ShapeDtypeStruct((seqs, dl), BF16),
        in_specs=[vmem] * 5 + [any_] * 3,
        out_specs=vmem,
        scratch_shapes=[
            pltpu.VMEM((width, hidden), BF16),
            pltpu.VMEM((width, hidden), BF16),
            pltpu.VMEM((hidden, width), BF16),
            pltpu.VMEM((lanes, seqs, width), BF16),
            pltpu.VMEM((groups, seqs, width + SIDE), BF16),
            pltpu.VMEM((lanes, seqs, dl), F32),
            pltpu.VMEM((lanes, zy, seqs, dl), BF16),
            pltpu.VMEM((lanes, zy, seqs, dl), BF16),
            pltpu.VMEM((lanes, zy, seqs, dl), F32),
            pltpu.VMEM((lanes, zy, seqs, dl), BF16),
            pltpu.VMEM((lanes, zy, seqs, dl), BF16),
            pltpu.VMEM((zy, seqs, dl), F32),
            pltpu.VMEM((zy, seqs, dl), BF16),
            pltpu.VMEM((zy, seqs, dl), BF16),
            pltpu.VMEM((lanes, zy, seqs, dl), BF16),
            pltpu.VMEM((lanes, zy, seqs, dl), BF16),
            pltpu.VMEM((nz, seqs, dl), BF16),
            pltpu.VMEM((nz, seqs, dl), BF16),
            dma((3,)),
            dma((lanes,)),
            dma((lanes,)),
            dma((2 * (nz // 2) ** 2 + 2 * nz * (ny - 1) + 2 * zy,)),
            dma((2, groups)),
            dma((lanes, nz)),
            dma((lanes, nz)),
            dma((lanes, nz)),
            dma((lanes, nz)),
            dma((ny, nz)),
            dma((ny, nz)),
            dma((nz,)),
            dma((nz,)),
        ],
        compiler_params=pltpu.CompilerParams(
            collective_id=0, has_side_effects=True, vmem_limit_bytes=60 * 1024 * 1024
        ),
    )(
        tokens, part, ffn_gain[None], routes.T, route_weight.T, expert_gate, expert_up, expert_down,
    )
    return mixed, new_state


def solution(mesh):
    return jax.shard_map(
        local,
        mesh=mesh,
        in_specs=(
            P("ep", None),
            P("ep", "tp", None, None),
            P(),
            P(None, "tp"),
            P(None, "tp"),
            P(None, "tp"),
            P(None, "tp"),
            P(),
            P(),
            P(),
            P(),
            P("tp", None),
            P(),
            P("ep", None),
            P("ep", None),
            P("ep", None, "tp"),
            P("ep", None, "tp"),
            P("ep", "tp", None),
        ),
        out_specs=(P("ep", "tp"), P("ep", "tp", None, None)),
        check_vma=False,
    )
```

```python
import functools

import jax
import jax.numpy as jnp
from jax import lax
from jax.experimental import pallas as pl
from jax.experimental.pallas import tpu as pltpu
from jax.sharding import PartitionSpec as P

EPS = 1e-06
MESH = pl.DeviceIdType.MESH
F32 = jnp.float32
BF16 = jnp.bfloat16
SIDE = 128


def silu(values):
    return values / (1.0 + jnp.exp(-values))


def unit_rows(values):
    return values * lax.rsqrt(jnp.sum(values * values, axis=-1, keepdims=True) + EPS)


def rms_scale(values, gain):
    return values * lax.rsqrt(jnp.mean(values * values, axis=-1, keepdims=True) + EPS) * gain


def mixer_kernel(
    tok_hbm, gain_hbm, bt_hbm, dt_hbm, rate_hbm, hg_hbm,
    wk_hbm, wq_hbm, wv_hbm, st_hbm, wz_hbm, wo_hbm,
    out_ref, ns_hbm,
    tok_ref, gain_ref, bt_ref, dt_ref, rate_ref, hg_ref,
    wk, wq, wv, wz, wo, st, ns, w_sem, s_sem, n_sem,
):
    heads, seqs, hd = st.shape[0], st.shape[1], st.shape[2]

    def fetch(src, dst, i):
        copy = pltpu.make_async_copy(src, dst, w_sem.at[i])
        copy.start()
        return copy

    small = (
        (tok_hbm, tok_ref), (gain_hbm, gain_ref), (bt_hbm, bt_ref),
        (dt_hbm, dt_ref), (rate_hbm, rate_ref), (hg_hbm, hg_ref),
    )
    first_in = [fetch(src, dst, 5 + i) for i, (src, dst) in enumerate(small)]
    ck, cq, cv = fetch(wk_hbm, wk, 0), fetch(wq_hbm, wq, 1), fetch(wv_hbm, wv, 2)
    cs = []
    for j in range(heads):
        copy = pltpu.make_async_copy(st_hbm.at[:, j], st.at[j], s_sem.at[j])
        copy.start()
        cs.append(copy)
    cz, co = fetch(wz_hbm, wz, 3), fetch(wo_hbm, wo, 4)

    for copy in first_in:
        copy.wait()
    normed = rms_scale(tok_ref[...].astype(F32), gain_ref[...]).astype(BF16)
    dims = (((1,), (1,)), ((), ()))
    bl = lax.dot_general(normed, bt_ref[...], dims, preferred_element_type=F32)
    dl = lax.dot_general(normed, dt_ref[...], dims, preferred_element_type=F32)
    strength = 1.0 / (1.0 + jnp.exp(-bl))
    softplus = jnp.maximum(dl, 0.0) + jnp.log1p(jnp.exp(-jnp.abs(dl)))
    fading = jnp.exp(-rate_ref[...] * softplus)
    first = lax.axis_index("tp") * heads
    head_ids = lax.broadcasted_iota(jnp.int32, bl.shape, 1)

    def own(values, j):
        return jnp.sum(jnp.where(head_ids == first + j, values, 0.0), axis=1, keepdims=True)

    def project(copy, ref):
        copy.wait()
        return jnp.dot(normed, ref[...], preferred_element_type=F32).astype(BF16).astype(F32)

    kp, qp, vp = project(ck, wk), project(cq, wq), project(cv, wv)
    row2 = lax.broadcasted_iota(jnp.int32, (2 * seqs, hd), 0)
    row1 = lax.broadcasted_iota(jnp.int32, (seqs, hd), 0)
    outs, readouts = [], []
    for j in range(heads):
        cut = slice(j * hd, (j + 1) * hd)
        kh = unit_rows(silu(kp[:, cut]))
        qh = unit_rows(silu(qp[:, cut])) * hd ** (-0.5)
        vh = silu(vp[:, cut])
        both = jnp.concatenate([kh, qh], axis=0)
        spread = jnp.concatenate(
            [jnp.where((row2 == t) | (row2 == t + seqs), both, 0.0).astype(BF16) for t in range(seqs)],
            axis=1,
        )
        cs[j].wait()
        held = st[j].reshape(seqs * hd, hd).astype(BF16)
        read = jnp.dot(spread, held, preferred_element_type=F32)
        fd, bt = own(fading, j), own(strength, j)
        delta = bt * (vh - fd * read[:seqs])
        readouts.append(fd * read[seqs:] + jnp.sum(kh * qh, axis=-1, keepdims=True) * delta)
        kt = kh.T.astype(BF16)
        fdb = jnp.broadcast_to(fd, (seqs, hd))
        step = 4
        for t0 in range(0, seqs, step):
            block = jnp.concatenate(
                [jnp.where(row1 == t, delta, 0.0).astype(BF16) for t in range(t0, t0 + step)], axis=1
            )
            written = jnp.dot(kt, block, preferred_element_type=F32)
            for i in range(step):
                t = t0 + i
                ns[j, t] = fdb[t : t + 1] * st[j, t] + written[:, i * hd : (i + 1) * hd]
        copy = pltpu.make_async_copy(ns.at[j], ns_hbm.at[:, j], n_sem.at[j])
        copy.start()
        outs.append(copy)
    zp = project(cz, wz)
    headed = jnp.concatenate(
        [
            (rms_scale(readouts[j], hg_ref[...]) * silu(zp[:, j * hd : (j + 1) * hd])).astype(BF16)
            for j in range(heads)
        ],
        axis=1,
    )
    co.wait()
    out_ref[...] = jnp.dot(headed, wo[...], preferred_element_type=F32).astype(BF16)
    for copy in outs:
        copy.wait()


def expert_kernel(
    nz, ny, lanes,
    tok_ref, part_ref, gain_ref, routes_ref, rw_ref, wg_hbm, wu_hbm, wd_hbm,
    out_ref,
    wg, wu, wd, tpb, rows, resid, cs, cr, pf, xs, xr, qf, ys, yr, ybs, ybr, zs, zr,
    w_sem, tp_s, tp_r, ag_s, ag_r, c_s, c_r, x_s, x_r, y_s, y_r, z_s, z_r,
):
    seqs, width = tok_ref.shape
    dl = width // lanes
    zy = nz * ny
    ep, tp = lax.axis_index("ep"), lax.axis_index("tp")
    c = lax.rem(ep, 2)
    y = lax.rem(ep // 2, ny)
    z = ep // (2 * ny)
    other = 1 - c

    fetched = []
    for i, (src, dst) in enumerate(((wg_hbm, wg), (wu_hbm, wu), (wd_hbm, wd))):
        copy = pltpu.make_async_copy(src.at[0], dst, w_sem.at[i])
        copy.start()
        fetched.append(copy)

    def device(zz, yy, cc):
        return {"ep": (zz * ny + yy) * 2 + cc}

    def turn(base, step, size):
        return lax.rem(base + step, size)

    partner = device(z, y, other)
    barrier = pltpu.get_barrier_semaphore()
    peers = [partner]
    peers += [{"tp": turn(tp, d, lanes)} for d in range(1, lanes)]
    peers += [device(z, turn(y, d, ny), c) for d in range(1, ny)]
    peers += [device(turn(z, d, nz), y, c) for d in range(1, nz)]
    for peer in peers:
        pl.semaphore_signal(barrier, inc=1, device_id=peer, device_id_type=MESH)
    pl.semaphore_wait(barrier, len(peers))

    started = []

    def remote(src, dst, s_sem, r_sem, dev):
        return pltpu.make_async_remote_copy(
            src_ref=src, dst_ref=dst, send_sem=s_sem, recv_sem=r_sem, device_id=dev, device_id_type=MESH
        )

    def send(src, dst, s_sem, r_sem, dev):
        copy = remote(src, dst, s_sem, r_sem, dev)
        copy.start()
        started.append(copy)

    def arrive(dst, s_sem, r_sem):
        remote(dst, dst, s_sem, r_sem, partner).wait_recv()

    for d in range(1, lanes):
        send(part_ref, tpb.at[tp], tp_s.at[d], tp_r.at[tp], {"tp": turn(tp, d, lanes)})

    routes, weights = routes_ref[...].astype(F32), rw_ref[...]
    top = routes.shape[0]
    pad = jnp.zeros((8 - 2 * top % 8, seqs), F32)
    turned = jnp.concatenate([routes, weights, pad], axis=0).T
    side = lax.broadcasted_iota(jnp.int32, (seqs, SIDE), 1)
    expert_of = jnp.where(side >= SIDE // 2, side - SIDE // 2, side).astype(F32)
    combine = jnp.zeros((seqs, SIDE), F32)
    for k in range(top):
        weight = turned[:, top + k : top + k + 1]
        combine = combine + jnp.where(expert_of == turned[:, k : k + 1], weight, 0.0)
    high = combine.astype(BF16).astype(F32)
    packed = jnp.where(side >= SIDE // 2, combine - high, high).astype(BF16)

    branch = part_ref[...].astype(F32)
    for d in range(1, lanes):
        src = turn(tp, d, lanes)
        arrive(tpb.at[src], tp_s.at[0], tp_r.at[src])
        branch = branch + tpb[src].astype(F32)
    res = (tok_ref[...].astype(F32) + branch.astype(BF16).astype(F32)).astype(BF16).astype(F32)
    for j in range(lanes):
        resid[j] = res[:, j * dl : (j + 1) * dl]

    def place(zz, yy, cc):
        return cc * zy + zz * ny + yy

    mine = place(z, y, c)
    rows[mine, :, :width] = rms_scale(res, gain_ref[...]).astype(BF16)
    rows[mine, :, width:] = packed

    count = [0]
    half = nz // 2
    low = z < half
    base = jnp.where(low, 0, half)
    edge = jnp.where(low, half - 1, half)
    far_edge = jnp.where(low, half, half - 1)
    outward = jnp.where(low, 1, -1)
    at_edge = z == edge
    middle = width // 2
    pieces = (slice(0, middle), slice(middle, width + SIDE))

    def block(p, piece):
        return rows.at[p, :, pieces[piece]]

    def pass_on(p, piece, dev):
        send(block(p, piece), block(p, piece), ag_s.at[count[0]], ag_r.at[piece, p], dev)
        count[0] += 1

    def landed(p, piece):
        arrive(block(p, piece), ag_s.at[0], ag_r.at[piece, p])

    def spread(p, piece):
        for d in range(1, ny):
            pass_on(p, piece, device(z, turn(y, d, ny), c))
        pass_on(p, piece, partner)

    mates = [base + lax.rem(z - base + d, half) for d in range(1, half)]
    both = range(len(pieces))
    for piece in both:
        pass_on(mine, piece, device(far_edge, y, c))
        for mate in mates:
            pass_on(mine, piece, device(mate, y, c))
        spread(mine, piece)
    for mate in mates:
        for piece in both:
            p = place(mate, y, c)
            landed(p, piece)
            spread(p, piece)
    relayed = []
    for i in range(half):
        for piece in both:
            p = place(far_edge + outward * i, y, c)
            landed(p, piece)
            for mate in mates:
                copy = remote(
                    block(p, piece), block(p, piece), ag_s.at[count[0]], ag_r.at[piece, p],
                    device(mate, y, c),
                )
                count[0] += 1
                relayed.append(copy)
                pl.when(at_edge)(copy.start)
            spread(p, piece)
    columns = [z] + mates + [far_edge + outward * i for i in range(half)]
    for zz in columns:
        for d in range(1, ny):
            for piece in both:
                p = place(zz, turn(y, d, ny), c)
                landed(p, piece)
                pass_on(p, piece, partner)

    my_expert = ep // 4
    lane_id = lax.broadcasted_iota(jnp.int32, (zy * seqs, SIDE), 1)

    def hidden_of(side_of):
        block = rows[pl.ds(side_of * zy, zy)].reshape(zy * seqs, width + SIDE)
        x = block[:, :width]
        pick = (lane_id == my_expert) | (lane_id == my_expert + SIDE // 2)
        share = jnp.sum(jnp.where(pick, block[:, width:].astype(F32), 0.0), axis=1, keepdims=True)
        gated = jnp.dot(x, wg[...], preferred_element_type=F32)
        lifted = jnp.dot(x, wu[...], preferred_element_type=F32)
        return (silu(gated) * lifted * share).astype(BF16)

    fetched[0].wait()
    fetched[1].wait()
    hidden_own = hidden_of(c)
    for d in range(ny):
        for zz in columns:
            for piece in both:
                landed(place(zz, turn(y, d, ny), other), piece)
    hidden_far = hidden_of(other)
    fetched[2].wait()
    targets = [lax.rem(z + outward * d + nz, nz) for d in range(nz - 1, -1, -1)]
    spans = [pl.ds(zt * ny, ny) for zt in targets]
    steps = range(nz)
    for j in range(lanes):
        cut = slice(j * dl, (j + 1) * dl)
        far = jnp.dot(hidden_far, wd[:, cut], preferred_element_type=F32)
        cs[j] = far.astype(BF16).reshape(zy, seqs, dl)
        for i in steps:
            send(cs.at[j, spans[i]], cr.at[j, spans[i]], c_s.at[j, i], c_r.at[j, i], partner)
    for j in range(lanes):
        cut = slice(j * dl, (j + 1) * dl)
        near_half = jnp.dot(hidden_own, wd[:, cut], preferred_element_type=F32)
        pf[j] = near_half.reshape(zy, seqs, dl)

    def first_tp(i):
        return i % 2 == 0

    tp_peers = [(d, turn(tp, d, lanes)) for d in range(1, lanes)]
    y_peers = [(d, turn(y, d, ny)) for d in range(1, ny)]
    for i in steps:
        zt, at = targets[i], spans[i]
        for j in range(lanes):
            arrive(cr.at[j, at], c_s.at[j, i], c_r.at[j, i])
        if first_tp(i):
            for d, jt in tp_peers:
                xs[jt, at] = (pf[jt, at] + cr[jt, at].astype(F32)).astype(BF16)
                send(xs.at[jt, at], xr.at[tp, at], x_s.at[d, i], x_r.at[tp, i], {"tp": jt})
            pf[tp, at] = pf[tp, at] + cr[tp, at].astype(F32)
        else:
            for d, yt in y_peers:
                row = zt * ny + yt
                ybs[:, row] = (pf[:, row] + cr[:, row].astype(F32)).astype(BF16)
                send(
                    ybs.at[:, row], ybr.at[:, zt * ny + y], y_s.at[d, i], y_r.at[y, i], device(z, yt, c)
                )
            row = zt * ny + y
            pf[:, row] = pf[:, row] + cr[:, row].astype(F32)
    for i in steps:
        zt, at = targets[i], spans[i]
        if first_tp(i):
            total = pf[tp, at]
            for d, src in tp_peers:
                arrive(xr.at[src, at], x_s.at[d, i], x_r.at[src, i])
                total = total + xr[src, at].astype(F32)
            qf[at] = total
            for d, yt in y_peers:
                row = zt * ny + yt
                ys[row] = qf[row].astype(BF16)
                send(ys.at[row], yr.at[zt * ny + y], y_s.at[d, i], y_r.at[y, i], device(z, yt, c))
        else:
            row = zt * ny + y
            total = pf[:, row]
            for d, src in y_peers:
                back = zt * ny + src
                arrive(ybr.at[:, back], y_s.at[d, i], y_r.at[src, i])
                total = total + ybr[:, back].astype(F32)
            pf[:, row] = total
            for d, jt in tp_peers:
                xs[jt, row] = pf[jt, row].astype(BF16)
                send(xs.at[jt, row], xr.at[tp, row], x_s.at[d, i], x_r.at[tp, i], {"tp": jt})
    for i in steps:
        zt = targets[i]
        row = zt * ny + y
        if first_tp(i):
            total = qf[row]
            for d, src in y_peers:
                back = zt * ny + src
                arrive(yr.at[back], y_s.at[d, i], y_r.at[src, i])
                total = total + yr[back].astype(F32)
        else:
            total = pf[tp, row]
            for d, src in tp_peers:
                arrive(xr.at[src, row], x_s.at[d, i], x_r.at[src, i])
                total = total + xr[src, row].astype(F32)
        if i < nz - 1:
            zs[zt] = total.astype(BF16)
            send(zs.at[zt], zr.at[z], z_s.at[i], z_r.at[z], device(zt, y, c))
    for d in range(1, nz):
        src = turn(z, d, nz)
        arrive(zr.at[src], z_s.at[0], z_r.at[src])
        total = total + zr[src].astype(F32)
    out_ref[...] = (resid[tp] + total).astype(BF16)
    for copy in started:
        copy.wait_send()
    for copy in relayed:
        pl.when(at_edge)(copy.wait_send)


def local(
    tokens, recur_state, attn_gain, query_weight, key_weight, value_weight, outgate_weight,
    beta_weight, decay_weight, decay_rate, head_gain, output_weight, ffn_gain, routes,
    route_weight, expert_gate, expert_up, expert_down,
):
    seqs, width = tokens.shape
    heads, hd = recur_state.shape[1], recur_state.shape[2]
    groups, lanes = lax.axis_size("ep"), lax.axis_size("tp")
    ny = 1
    while ny * ny * 4 <= groups // 2:
        ny *= 2
    nz = groups // (2 * ny)
    zy = nz * ny
    dl = width // lanes
    hidden = expert_gate.shape[2]
    vmem = pl.BlockSpec(memory_space=pltpu.VMEM)
    any_ = pl.BlockSpec(memory_space=pl.ANY)
    dma = pltpu.SemaphoreType.DMA
    inner = heads * hd
    smalls = (
        tokens, attn_gain[None], beta_weight.T, decay_weight.T, decay_rate[None], head_gain[None],
    )
    part, new_state = pl.pallas_call(
        mixer_kernel,
        name="mixer",
        out_shape=(
            pltpu.VMEM((seqs, width), BF16),
            jax.ShapeDtypeStruct(recur_state.shape, F32),
        ),
        in_specs=[any_] * 12,
        out_specs=(vmem, any_),
        scratch_shapes=[pltpu.VMEM(small.shape, small.dtype) for small in smalls]
        + [pltpu.VMEM((width, inner), BF16)] * 4
        + [
            pltpu.VMEM((inner, width), BF16),
            pltpu.VMEM((heads, seqs, hd, hd), F32),
            pltpu.VMEM((heads, seqs, hd, hd), F32),
            dma((5 + len(smalls),)),
            dma((heads,)),
            dma((heads,)),
        ],
        compiler_params=pltpu.CompilerParams(vmem_limit_bytes=60 * 1024 * 1024),
    )(
        *smalls, key_weight, query_weight, value_weight, recur_state, outgate_weight, output_weight,
    )
    mixed = pl.pallas_call(
        functools.partial(expert_kernel, nz, ny, lanes),
        name="experts",
        out_shape=pltpu.VMEM((seqs, dl), BF16),
        in_specs=[vmem] * 5 + [any_] * 3,
        out_specs=vmem,
        scratch_shapes=[
            pltpu.VMEM((width, hidden), BF16),
            pltpu.VMEM((width, hidden), BF16),
            pltpu.VMEM((hidden, width), BF16),
            pltpu.VMEM((lanes, seqs, width), BF16),
            pltpu.VMEM((groups, seqs, width + SIDE), BF16),
            pltpu.VMEM((lanes, seqs, dl), F32),
            pltpu.VMEM((lanes, zy, seqs, dl), BF16),
            pltpu.VMEM((lanes, zy, seqs, dl), BF16),
            pltpu.VMEM((lanes, zy, seqs, dl), F32),
            pltpu.VMEM((lanes, zy, seqs, dl), BF16),
            pltpu.VMEM((lanes, zy, seqs, dl), BF16),
            pltpu.VMEM((zy, seqs, dl), F32),
            pltpu.VMEM((zy, seqs, dl), BF16),
            pltpu.VMEM((zy, seqs, dl), BF16),
            pltpu.VMEM((lanes, zy, seqs, dl), BF16),
            pltpu.VMEM((lanes, zy, seqs, dl), BF16),
            pltpu.VMEM((nz, seqs, dl), BF16),
            pltpu.VMEM((nz, seqs, dl), BF16),
            dma((3,)),
            dma((lanes,)),
            dma((lanes,)),
            dma((2 * (nz // 2) ** 2 + 2 * nz * (ny - 1) + 2 * zy,)),
            dma((2, groups)),
            dma((lanes, nz)),
            dma((lanes, nz)),
            dma((lanes, nz)),
            dma((lanes, nz)),
            dma((ny, nz)),
            dma((ny, nz)),
            dma((nz,)),
            dma((nz,)),
        ],
        compiler_params=pltpu.CompilerParams(
            collective_id=0, has_side_effects=True, vmem_limit_bytes=60 * 1024 * 1024
        ),
    )(
        tokens, pltpu.with_memory_space_constraint(part, pltpu.VMEM), ffn_gain[None], routes.T, route_weight.T, expert_gate, expert_up, expert_down,
    )
    return mixed, new_state


def solution(mesh):
    return jax.shard_map(
        local,
        mesh=mesh,
        in_specs=(
            P("ep", None),
            P("ep", "tp", None, None),
            P(),
            P(None, "tp"),
            P(None, "tp"),
            P(None, "tp"),
            P(None, "tp"),
            P(),
            P(),
            P(),
            P(),
            P("tp", None),
            P(),
            P("ep", None),
            P("ep", None),
            P("ep", None, "tp"),
            P("ep", None, "tp"),
            P("ep", "tp", None),
        ),
        out_specs=(P("ep", "tp"), P("ep", "tp", None, None)),
        check_vma=False,
    )
```

```python
import functools

import jax
import jax.numpy as jnp
from jax import lax
from jax.experimental import pallas as pl
from jax.experimental.pallas import tpu as pltpu
from jax.sharding import PartitionSpec as P

EPS = 1e-06
MESH = pl.DeviceIdType.MESH
F32 = jnp.float32
BF16 = jnp.bfloat16
SIDE = 128


def silu(values):
    return values / (1.0 + jnp.exp(-values))


def unit_rows(values):
    return values * lax.rsqrt(jnp.sum(values * values, axis=-1, keepdims=True) + EPS)


def rms_scale(values, gain):
    return values * lax.rsqrt(jnp.mean(values * values, axis=-1, keepdims=True) + EPS) * gain


def mixer_kernel(
    tok_hbm, gain_hbm, bt_hbm, dt_hbm, rate_hbm, hg_hbm,
    wk_hbm, wq_hbm, wv_hbm, st_hbm, wz_hbm, wo_hbm,
    out_ref, ns_hbm,
    tok_ref, gain_ref, bt_ref, dt_ref, rate_ref, hg_ref,
    wk, wq, wv, wz, wo, st, ns, w_sem, s_sem, n_sem,
):
    heads, seqs, hd = st.shape[0], st.shape[1], st.shape[2]

    def fetch(src, dst, i):
        copy = pltpu.make_async_copy(src, dst, w_sem.at[i])
        copy.start()
        return copy

    small = (
        (tok_hbm, tok_ref), (gain_hbm, gain_ref), (bt_hbm, bt_ref),
        (dt_hbm, dt_ref), (rate_hbm, rate_ref), (hg_hbm, hg_ref),
    )
    first_in = [fetch(src, dst, 5 + i) for i, (src, dst) in enumerate(small)]
    ck, cq, cv = fetch(wk_hbm, wk, 0), fetch(wq_hbm, wq, 1), fetch(wv_hbm, wv, 2)
    cs = []
    for j in range(heads):
        copy = pltpu.make_async_copy(st_hbm.at[:, j], st.at[j], s_sem.at[j])
        copy.start()
        cs.append(copy)
    cz, co = fetch(wz_hbm, wz, 3), fetch(wo_hbm, wo, 4)

    for copy in first_in:
        copy.wait()
    normed = rms_scale(tok_ref[...].astype(F32), gain_ref[...]).astype(BF16)
    dims = (((1,), (1,)), ((), ()))
    bl = lax.dot_general(normed, bt_ref[...], dims, preferred_element_type=F32)
    dl = lax.dot_general(normed, dt_ref[...], dims, preferred_element_type=F32)
    strength = 1.0 / (1.0 + jnp.exp(-bl))
    softplus = jnp.maximum(dl, 0.0) + jnp.log1p(jnp.exp(-jnp.abs(dl)))
    fading = jnp.exp(-rate_ref[...] * softplus)
    first = lax.axis_index("tp") * heads
    head_ids = lax.broadcasted_iota(jnp.int32, bl.shape, 1)

    def own(values, j):
        return jnp.sum(jnp.where(head_ids == first + j, values, 0.0), axis=1, keepdims=True)

    def project(copy, ref):
        copy.wait()
        return jnp.dot(normed, ref[...], preferred_element_type=F32).astype(BF16).astype(F32)

    kp, qp, vp = project(ck, wk), project(cq, wq), project(cv, wv)
    row2 = lax.broadcasted_iota(jnp.int32, (2 * seqs, hd), 0)
    row1 = lax.broadcasted_iota(jnp.int32, (seqs, hd), 0)
    outs, readouts = [], []
    for j in range(heads):
        cut = slice(j * hd, (j + 1) * hd)
        kh = unit_rows(silu(kp[:, cut]))
        qh = unit_rows(silu(qp[:, cut])) * hd ** (-0.5)
        vh = silu(vp[:, cut])
        both = jnp.concatenate([kh, qh], axis=0)
        spread = jnp.concatenate(
            [jnp.where((row2 == t) | (row2 == t + seqs), both, 0.0).astype(BF16) for t in range(seqs)],
            axis=1,
        )
        cs[j].wait()
        held = st[j].reshape(seqs * hd, hd).astype(BF16)
        read = jnp.dot(spread, held, preferred_element_type=F32)
        fd, bt = own(fading, j), own(strength, j)
        delta = bt * (vh - fd * read[:seqs])
        readouts.append(fd * read[seqs:] + jnp.sum(kh * qh, axis=-1, keepdims=True) * delta)
        kt = kh.T.astype(BF16)
        fdb = jnp.broadcast_to(fd, (seqs, hd))
        step = 4
        for t0 in range(0, seqs, step):
            block = jnp.concatenate(
                [jnp.where(row1 == t, delta, 0.0).astype(BF16) for t in range(t0, t0 + step)], axis=1
            )
            written = jnp.dot(kt, block, preferred_element_type=F32)
            for i in range(step):
                t = t0 + i
                ns[j, t] = fdb[t : t + 1] * st[j, t] + written[:, i * hd : (i + 1) * hd]
        copy = pltpu.make_async_copy(ns.at[j], ns_hbm.at[:, j], n_sem.at[j])
        copy.start()
        outs.append(copy)
    zp = project(cz, wz)
    headed = jnp.concatenate(
        [
            (rms_scale(readouts[j], hg_ref[...]) * silu(zp[:, j * hd : (j + 1) * hd])).astype(BF16)
            for j in range(heads)
        ],
        axis=1,
    )
    co.wait()
    out_ref[...] = jnp.dot(headed, wo[...], preferred_element_type=F32).astype(BF16)
    for copy in outs:
        copy.wait()


def expert_kernel(
    nz, ny, lanes,
    part_ref, tok_hbm, gain_hbm, routes_hbm, rw_hbm, wg_hbm, wu_hbm, wd_hbm,
    out_ref,
    tok_ref, gain_ref, routes_ref, rw_ref,
    wg, wu, wd, tpb, rows, resid, cs, cr, pf, xs, xr, qf, ys, yr, ybs, ybr, zs, zr,
    w_sem, tp_s, tp_r, ag_s, ag_r, c_s, c_r, x_s, x_r, y_s, y_r, z_s, z_r,
):
    seqs, width = tok_ref.shape
    dl = width // lanes
    zy = nz * ny
    ep, tp = lax.axis_index("ep"), lax.axis_index("tp")
    c = lax.rem(ep, 2)
    y = lax.rem(ep // 2, ny)
    z = ep // (2 * ny)
    other = 1 - c

    small = (
        (tok_hbm, tok_ref), (gain_hbm, gain_ref), (routes_hbm, routes_ref), (rw_hbm, rw_ref),
    )
    first_in = []
    for i, (src, dst) in enumerate(small):
        copy = pltpu.make_async_copy(src, dst, w_sem.at[3 + i])
        copy.start()
        first_in.append(copy)
    fetched = []
    for i, (src, dst) in enumerate(((wg_hbm, wg), (wu_hbm, wu), (wd_hbm, wd))):
        copy = pltpu.make_async_copy(src.at[0], dst, w_sem.at[i])
        copy.start()
        fetched.append(copy)

    def device(zz, yy, cc):
        return {"ep": (zz * ny + yy) * 2 + cc}

    def turn(base, step, size):
        return lax.rem(base + step, size)

    partner = device(z, y, other)
    barrier = pltpu.get_barrier_semaphore()
    peers = [partner]
    peers += [{"tp": turn(tp, d, lanes)} for d in range(1, lanes)]
    peers += [device(z, turn(y, d, ny), c) for d in range(1, ny)]
    peers += [device(turn(z, d, nz), y, c) for d in range(1, nz)]
    for peer in peers:
        pl.semaphore_signal(barrier, inc=1, device_id=peer, device_id_type=MESH)
    pl.semaphore_wait(barrier, len(peers))

    started = []

    def remote(src, dst, s_sem, r_sem, dev):
        return pltpu.make_async_remote_copy(
            src_ref=src, dst_ref=dst, send_sem=s_sem, recv_sem=r_sem, device_id=dev, device_id_type=MESH
        )

    def send(src, dst, s_sem, r_sem, dev):
        copy = remote(src, dst, s_sem, r_sem, dev)
        copy.start()
        started.append(copy)

    def arrive(dst, s_sem, r_sem):
        remote(dst, dst, s_sem, r_sem, partner).wait_recv()

    for d in range(1, lanes):
        send(part_ref, tpb.at[tp], tp_s.at[d], tp_r.at[tp], {"tp": turn(tp, d, lanes)})

    for copy in first_in:
        copy.wait()
    routes, weights = routes_ref[...].astype(F32), rw_ref[...]
    top = routes.shape[0]
    pad = jnp.zeros((8 - 2 * top % 8, seqs), F32)
    turned = jnp.concatenate([routes, weights, pad], axis=0).T
    side = lax.broadcasted_iota(jnp.int32, (seqs, SIDE), 1)
    expert_of = jnp.where(side >= SIDE // 2, side - SIDE // 2, side).astype(F32)
    combine = jnp.zeros((seqs, SIDE), F32)
    for k in range(top):
        weight = turned[:, top + k : top + k + 1]
        combine = combine + jnp.where(expert_of == turned[:, k : k + 1], weight, 0.0)
    high = combine.astype(BF16).astype(F32)
    packed = jnp.where(side >= SIDE // 2, combine - high, high).astype(BF16)

    branch = part_ref[...].astype(F32)
    for d in range(1, lanes):
        src = turn(tp, d, lanes)
        arrive(tpb.at[src], tp_s.at[0], tp_r.at[src])
        branch = branch + tpb[src].astype(F32)
    res = (tok_ref[...].astype(F32) + branch.astype(BF16).astype(F32)).astype(BF16).astype(F32)
    for j in range(lanes):
        resid[j] = res[:, j * dl : (j + 1) * dl]

    def place(zz, yy, cc):
        return cc * zy + zz * ny + yy

    mine = place(z, y, c)
    rows[mine, :, :width] = rms_scale(res, gain_ref[...]).astype(BF16)
    rows[mine, :, width:] = packed

    count = [0]
    half = nz // 2
    low = z < half
    base = jnp.where(low, 0, half)
    edge = jnp.where(low, half - 1, half)
    far_edge = jnp.where(low, half, half - 1)
    outward = jnp.where(low, 1, -1)
    at_edge = z == edge
    middle = width // 2
    pieces = (slice(0, middle), slice(middle, width + SIDE))

    def block(p, piece):
        return rows.at[p, :, pieces[piece]]

    def pass_on(p, piece, dev):
        send(block(p, piece), block(p, piece), ag_s.at[count[0]], ag_r.at[piece, p], dev)
        count[0] += 1

    def landed(p, piece):
        arrive(block(p, piece), ag_s.at[0], ag_r.at[piece, p])

    def spread(p, piece):
        for d in range(1, ny):
            pass_on(p, piece, device(z, turn(y, d, ny), c))
        pass_on(p, piece, partner)

    mates = [base + lax.rem(z - base + d, half) for d in range(1, half)]
    both = range(len(pieces))
    for piece in both:
        pass_on(mine, piece, device(far_edge, y, c))
        for mate in mates:
            pass_on(mine, piece, device(mate, y, c))
        spread(mine, piece)
    for mate in mates:
        for piece in both:
            p = place(mate, y, c)
            landed(p, piece)
            spread(p, piece)
    relayed = []
    for i in range(half):
        for piece in both:
            p = place(far_edge + outward * i, y, c)
            landed(p, piece)
            for mate in mates:
                copy = remote(
                    block(p, piece), block(p, piece), ag_s.at[count[0]], ag_r.at[piece, p],
                    device(mate, y, c),
                )
                count[0] += 1
                relayed.append(copy)
                pl.when(at_edge)(copy.start)
            spread(p, piece)
    columns = [z] + mates + [far_edge + outward * i for i in range(half)]
    for zz in columns:
        for d in range(1, ny):
            for piece in both:
                p = place(zz, turn(y, d, ny), c)
                landed(p, piece)
                pass_on(p, piece, partner)

    my_expert = ep // 4
    lane_id = lax.broadcasted_iota(jnp.int32, (zy * seqs, SIDE), 1)

    def hidden_of(side_of):
        block = rows[pl.ds(side_of * zy, zy)].reshape(zy * seqs, width + SIDE)
        x = block[:, :width]
        pick = (lane_id == my_expert) | (lane_id == my_expert + SIDE // 2)
        share = jnp.sum(jnp.where(pick, block[:, width:].astype(F32), 0.0), axis=1, keepdims=True)
        gated = jnp.dot(x, wg[...], preferred_element_type=F32)
        lifted = jnp.dot(x, wu[...], preferred_element_type=F32)
        return (silu(gated) * lifted * share).astype(BF16)

    fetched[0].wait()
    fetched[1].wait()
    hidden_own = hidden_of(c)
    for d in range(ny):
        for zz in columns:
            for piece in both:
                landed(place(zz, turn(y, d, ny), other), piece)
    hidden_far = hidden_of(other)
    fetched[2].wait()
    targets = [lax.rem(z + outward * d + nz, nz) for d in range(nz - 1, -1, -1)]
    spans = [pl.ds(zt * ny, ny) for zt in targets]
    steps = range(nz)
    for j in range(lanes):
        cut = slice(j * dl, (j + 1) * dl)
        far = jnp.dot(hidden_far, wd[:, cut], preferred_element_type=F32)
        cs[j] = far.astype(BF16).reshape(zy, seqs, dl)
        for i in steps:
            send(cs.at[j, spans[i]], cr.at[j, spans[i]], c_s.at[j, i], c_r.at[j, i], partner)
    for j in range(lanes):
        cut = slice(j * dl, (j + 1) * dl)
        near_half = jnp.dot(hidden_own, wd[:, cut], preferred_element_type=F32)
        pf[j] = near_half.reshape(zy, seqs, dl)

    def first_tp(i):
        return i % 2 == 0

    tp_peers = [(d, turn(tp, d, lanes)) for d in range(1, lanes)]
    y_peers = [(d, turn(y, d, ny)) for d in range(1, ny)]
    for i in steps:
        zt, at = targets[i], spans[i]
        for j in range(lanes):
            arrive(cr.at[j, at], c_s.at[j, i], c_r.at[j, i])
        if first_tp(i):
            for d, jt in tp_peers:
                xs[jt, at] = (pf[jt, at] + cr[jt, at].astype(F32)).astype(BF16)
                send(xs.at[jt, at], xr.at[tp, at], x_s.at[d, i], x_r.at[tp, i], {"tp": jt})
            pf[tp, at] = pf[tp, at] + cr[tp, at].astype(F32)
        else:
            for d, yt in y_peers:
                row = zt * ny + yt
                ybs[:, row] = (pf[:, row] + cr[:, row].astype(F32)).astype(BF16)
                send(
                    ybs.at[:, row], ybr.at[:, zt * ny + y], y_s.at[d, i], y_r.at[y, i], device(z, yt, c)
                )
            row = zt * ny + y
            pf[:, row] = pf[:, row] + cr[:, row].astype(F32)
    for i in steps:
        zt, at = targets[i], spans[i]
        if first_tp(i):
            total = pf[tp, at]
            for d, src in tp_peers:
                arrive(xr.at[src, at], x_s.at[d, i], x_r.at[src, i])
                total = total + xr[src, at].astype(F32)
            qf[at] = total
            for d, yt in y_peers:
                row = zt * ny + yt
                ys[row] = qf[row].astype(BF16)
                send(ys.at[row], yr.at[zt * ny + y], y_s.at[d, i], y_r.at[y, i], device(z, yt, c))
        else:
            row = zt * ny + y
            total = pf[:, row]
            for d, src in y_peers:
                back = zt * ny + src
                arrive(ybr.at[:, back], y_s.at[d, i], y_r.at[src, i])
                total = total + ybr[:, back].astype(F32)
            pf[:, row] = total
            for d, jt in tp_peers:
                xs[jt, row] = pf[jt, row].astype(BF16)
                send(xs.at[jt, row], xr.at[tp, row], x_s.at[d, i], x_r.at[tp, i], {"tp": jt})
    for i in steps:
        zt = targets[i]
        row = zt * ny + y
        if first_tp(i):
            total = qf[row]
            for d, src in y_peers:
                back = zt * ny + src
                arrive(yr.at[back], y_s.at[d, i], y_r.at[src, i])
                total = total + yr[back].astype(F32)
        else:
            total = pf[tp, row]
            for d, src in tp_peers:
                arrive(xr.at[src, row], x_s.at[d, i], x_r.at[src, i])
                total = total + xr[src, row].astype(F32)
        if i < nz - 1:
            zs[zt] = total.astype(BF16)
            send(zs.at[zt], zr.at[z], z_s.at[i], z_r.at[z], device(zt, y, c))
    for d in range(1, nz):
        src = turn(z, d, nz)
        arrive(zr.at[src], z_s.at[0], z_r.at[src])
        total = total + zr[src].astype(F32)
    out_ref[...] = (resid[tp] + total).astype(BF16)
    for copy in started:
        copy.wait_send()
    for copy in relayed:
        pl.when(at_edge)(copy.wait_send)


def local(
    tokens, recur_state, attn_gain, query_weight, key_weight, value_weight, outgate_weight,
    beta_weight, decay_weight, decay_rate, head_gain, output_weight, ffn_gain, routes,
    route_weight, expert_gate, expert_up, expert_down,
):
    seqs, width = tokens.shape
    heads, hd = recur_state.shape[1], recur_state.shape[2]
    groups, lanes = lax.axis_size("ep"), lax.axis_size("tp")
    ny = 1
    while ny * ny * 4 <= groups // 2:
        ny *= 2
    nz = groups // (2 * ny)
    zy = nz * ny
    dl = width // lanes
    hidden = expert_gate.shape[2]
    vmem = pl.BlockSpec(memory_space=pltpu.VMEM)
    any_ = pl.BlockSpec(memory_space=pl.ANY)
    dma = pltpu.SemaphoreType.DMA
    inner = heads * hd
    smalls = (
        tokens, attn_gain[None], beta_weight.T, decay_weight.T, decay_rate[None], head_gain[None],
    )
    part, new_state = pl.pallas_call(
        mixer_kernel,
        name="mixer",
        out_shape=(
            pltpu.VMEM((seqs, width), BF16),
            jax.ShapeDtypeStruct(recur_state.shape, F32),
        ),
        in_specs=[any_] * 12,
        out_specs=(vmem, any_),
        scratch_shapes=[pltpu.VMEM(small.shape, small.dtype) for small in smalls]
        + [pltpu.VMEM((width, inner), BF16)] * 4
        + [
            pltpu.VMEM((inner, width), BF16),
            pltpu.VMEM((heads, seqs, hd, hd), F32),
            pltpu.VMEM((heads, seqs, hd, hd), F32),
            dma((5 + len(smalls),)),
            dma((heads,)),
            dma((heads,)),
        ],
        compiler_params=pltpu.CompilerParams(vmem_limit_bytes=60 * 1024 * 1024),
    )(
        *smalls, key_weight, query_weight, value_weight, recur_state, outgate_weight, output_weight,
    )
    smalls = (tokens, ffn_gain[None], routes.T, route_weight.T)
    mixed = pl.pallas_call(
        functools.partial(expert_kernel, nz, ny, lanes),
        name="experts",
        out_shape=pltpu.VMEM((seqs, dl), BF16),
        in_specs=[vmem] + [any_] * 7,
        out_specs=vmem,
        scratch_shapes=[pltpu.VMEM(small.shape, small.dtype) for small in smalls]
        + [
            pltpu.VMEM((width, hidden), BF16),
            pltpu.VMEM((width, hidden), BF16),
            pltpu.VMEM((hidden, width), BF16),
            pltpu.VMEM((lanes, seqs, width), BF16),
            pltpu.VMEM((groups, seqs, width + SIDE), BF16),
            pltpu.VMEM((lanes, seqs, dl), F32),
            pltpu.VMEM((lanes, zy, seqs, dl), BF16),
            pltpu.VMEM((lanes, zy, seqs, dl), BF16),
            pltpu.VMEM((lanes, zy, seqs, dl), F32),
            pltpu.VMEM((lanes, zy, seqs, dl), BF16),
            pltpu.VMEM((lanes, zy, seqs, dl), BF16),
            pltpu.VMEM((zy, seqs, dl), F32),
            pltpu.VMEM((zy, seqs, dl), BF16),
            pltpu.VMEM((zy, seqs, dl), BF16),
            pltpu.VMEM((lanes, zy, seqs, dl), BF16),
            pltpu.VMEM((lanes, zy, seqs, dl), BF16),
            pltpu.VMEM((nz, seqs, dl), BF16),
            pltpu.VMEM((nz, seqs, dl), BF16),
            dma((3 + len(smalls),)),
            dma((lanes,)),
            dma((lanes,)),
            dma((2 * (nz // 2) ** 2 + 2 * nz * (ny - 1) + 2 * zy,)),
            dma((2, groups)),
            dma((lanes, nz)),
            dma((lanes, nz)),
            dma((lanes, nz)),
            dma((lanes, nz)),
            dma((ny, nz)),
            dma((ny, nz)),
            dma((nz,)),
            dma((nz,)),
        ],
        compiler_params=pltpu.CompilerParams(
            collective_id=0, has_side_effects=True, vmem_limit_bytes=60 * 1024 * 1024
        ),
    )(
        pltpu.with_memory_space_constraint(part, pltpu.VMEM), *smalls, expert_gate, expert_up, expert_down,
    )
    return mixed, new_state


def solution(mesh):
    return jax.shard_map(
        local,
        mesh=mesh,
        in_specs=(
            P("ep", None),
            P("ep", "tp", None, None),
            P(),
            P(None, "tp"),
            P(None, "tp"),
            P(None, "tp"),
            P(None, "tp"),
            P(),
            P(),
            P(),
            P(),
            P("tp", None),
            P(),
            P("ep", None),
            P("ep", None),
            P("ep", None, "tp"),
            P("ep", None, "tp"),
            P("ep", "tp", None),
        ),
        out_specs=(P("ep", "tp"), P("ep", "tp", None, None)),
        check_vma=False,
    )
```
